32 devices in a mesh: sp: 4 (over z), fs: 4 (over y, x), tp: 2 (over core).
Axes of the slice: x: 2, y: 2, z: 4, core: 2. Of those that a mesh axis runs over, the one named last changes fastest.
Arguments:
- tokens: bfloat16 [4, 1024, 2048], P('fs', 'sp', 'tp'), may hold values from -6 to 6
- norm_gain: float32 [2048], replicated, may hold values from 0.1 to 1.9
- ret_query: bfloat16 [2048, 1024], P('sp', 'tp'), may hold values from -0.125 to 0.125
- ret_key: bfloat16 [2048, 1024], P('sp', 'tp'), may hold values from -0.125 to 0.125
- ret_value: bfloat16 [2048, 1024], P('sp', 'tp'), may hold values from -0.125 to 0.125
- att_query: bfloat16 [2048, 1024], P('sp', 'tp'), may hold values from -0.125 to 0.125
- att_key: bfloat16 [2048, 256], P('sp', 'tp'), may hold values from -0.125 to 0.125
- att_value: bfloat16 [2048, 256], P('sp', 'tp'), may hold values from -0.125 to 0.125
- log_decay: float32 [4, 4, 1024], P('fs', 'tp', 'sp'), may hold values from -1 to 0
- start_state: float32 [4, 4, 256, 256], P('fs', 'tp'), may hold values from -12 to 12
- ret_gain: float32 [1024], P('tp'), may hold values from 0.1 to 1.9
- sink_logits: float32 [16], P('tp'), may hold values from 1 to 5
- ret_out: bfloat16 [1024, 2048], P('tp', 'fs'), may hold values from -0.1875 to 0.1875
- att_out: bfloat16 [1024, 2048], P('tp', 'fs'), may hold values from -1.5 to 1.5
Outputs:
- mixed: bfloat16 [4, 1024, 2048], P('fs', 'sp', 'tp')
The draws below stay inside these ranges and needn't reach their ends.
All inputs are finite; a program needn't handle non-finite values.
Results may differ from the reference program's by a relative error of at most 0.015.
Values may be sent and summed in bfloat16 or wider, within the bound.
No kernel may reach another device: no remote copies, remote signals or barrier semaphores. Data moves between devices by JAX's collectives and lax.ppermute only.
A program may use at most 128 MiB of HBM per device.

```python
import jax
import jax.numpy as jnp
from jax import lax

D = 2048
RETENTION_HEADS = 4
DK = 256
DV = 256
AQH = 16
AKH = 4
HD = 64
WINDOW = 128
BLOCK = 128
TOK_DEV = 256
SEQUENCE_COUNT = 4
SEQUENCE_LENGTH = 1024
N_TP = 2


def draw_log_decay(key, part):
    random_subkeys = jax.random.split(jax.random.fold_in(key, 17), 5)
    blocks = SEQUENCE_LENGTH // TOK_DEV
    ranking = jax.vmap(lambda inner: jax.random.permutation(inner, RETENTION_HEADS))(jax.random.split(random_subkeys[0], SEQUENCE_COUNT))
    fast_heads = (ranking < RETENTION_HEADS // 2).astype(jnp.float32)
    baseline_decay = fast_heads * (3.0 / BLOCK) + (1.0 - fast_heads) * (1.0 / SEQUENCE_LENGTH)
    noise_spread = jax.random.uniform(random_subkeys[1], (SEQUENCE_COUNT, RETENTION_HEADS, blocks), jnp.float32, 0.4, 1.2)
    noise_spread = jnp.repeat(noise_spread, TOK_DEV, axis=-1)
    random_noise = jax.random.uniform(random_subkeys[2], (SEQUENCE_COUNT, RETENTION_HEADS, SEQUENCE_LENGTH), jnp.float32, 0.5, 1.5)
    spike_position = jax.random.randint(random_subkeys[3], (SEQUENCE_COUNT, RETENTION_HEADS, 2), 0, SEQUENCE_LENGTH)
    spike_magnitude = jax.random.uniform(random_subkeys[4], (SEQUENCE_COUNT, RETENTION_HEADS, 2), jnp.float32, 0.2, 0.4)
    position_list = jnp.arange(SEQUENCE_LENGTH, dtype=jnp.int32)
    spike_events = jnp.sum(jnp.where(position_list[None, None, None, :] == spike_position[..., None], jnp.log(1.0 - spike_magnitude)[..., None], 0.0), axis=2)
    return (-baseline_decay[..., None] * noise_spread * random_noise + spike_events).astype(jnp.float32)


def levels(rng, dims, cuts, smallest, high):
    level, own = 1.0, jax.random.fold_in(rng, 6)
    for axis_at, blocks in cuts:
        heights = jnp.exp(jax.random.uniform(jax.random.fold_in(own, axis_at), (blocks,), jnp.float32, smallest / len(cuts), high / len(cuts)))
        level = level * jnp.repeat(heights, dims[axis_at] // blocks).reshape([-1 if axis == axis_at else 1 for axis in range(len(dims))])
    return level


def gaussian(stream_key, dims, deviation, bound, cuts=(), kind=jnp.bfloat16):
    drawn = jax.random.normal(stream_key, dims, jnp.float32) * deviation
    if len(cuts) > 0:
        drawn = levels(stream_key, dims, cuts, -0.22, 0.18) * drawn
    return jnp.clip(drawn, min=-bound, max=bound).astype(kind)


def setup_inputs(seed: int = 0) -> dict:
    key_of = jax.random.split(jax.random.key(seed), 15)
    return {
        "tokens": gaussian(key_of[0], (SEQUENCE_COUNT, SEQUENCE_LENGTH, D), 1.0, 6.0, ((0, 4), (1, 4), (2, 2))),
        "norm_gain": jnp.clip(1.0 + 0.18 * jax.random.normal(key_of[1], (D,), jnp.float32), 0.1, 1.9),
        "ret_query": gaussian(key_of[2], (D, RETENTION_HEADS * DK), D ** -0.5, 0.125, ((0, 4), (1, 2))),
        "ret_key": gaussian(key_of[3], (D, RETENTION_HEADS * DK), D ** -0.5, 0.125, ((0, 4), (1, 2))),
        "ret_value": gaussian(key_of[4], (D, RETENTION_HEADS * DV), D ** -0.5, 0.125, ((0, 4), (1, 2))),
        "att_query": gaussian(key_of[5], (D, AQH * HD), D ** -0.5, 0.125, ((0, 4), (1, 2))),
        "att_key": gaussian(key_of[6], (D, AKH * HD), D ** -0.5, 0.125, ((0, 4), (1, 2))),
        "att_value": gaussian(key_of[7], (D, AKH * HD), D ** -0.5, 0.125, ((0, 4), (1, 2))),
        "log_decay": draw_log_decay(jax.random.fold_in(key_of[14], 71), 0),
        "start_state": gaussian(key_of[9], (SEQUENCE_COUNT, RETENTION_HEADS, DK, DV), (2 * (TOK_DEV // DK) ** 0.5), 12.0, ((0, 4), (1, 2)), jnp.float32),
        "ret_gain": jnp.clip(1.0 + 0.18 * jax.random.normal(key_of[10], (RETENTION_HEADS * DV,), jnp.float32), 0.1, 1.9),
        "sink_logits": jnp.clip(1.0 + 4.0 * jax.random.uniform(key_of[11], (AQH,), jnp.float32) ** levels(key_of[11], (AQH,), ((0, 2),), -0.2, 0.2), 1.0, 5.0),
        "ret_out": gaussian(key_of[12], (RETENTION_HEADS * DV, D), (RETENTION_HEADS * DV) ** -0.5, 0.1875, ((0, 2), (1, 4))),
        "att_out": gaussian(key_of[13], (AQH * HD, D), (AQH * HD // 64) ** -0.5, 1.5, ((0, 2), (1, 4))),
    }


epsilon = 1e-06
exact_result = lax.Precision.HIGHEST

def rotate(values, positions):
    half_dim = values.shape[-1] // 2
    inverse = 1.0 / 10000.0 ** (jnp.arange(half_dim, dtype=jnp.float32) / half_dim)
    angles = positions.astype(jnp.float32)[:, None] * inverse[None, :]
    cosine = jnp.cos(angles)[:, None, :]
    sine_table = jnp.sin(angles)[:, None, :]
    front_half = values[..., :half_dim]
    back_half = values[..., half_dim:]
    return jnp.concatenate([front_half * cosine - back_half * sine_table, front_half * sine_table + back_half * cosine], axis=-1)

def block_step(memory_state, inputs):
    queries, key_matrix_rows, value_matrix_rows, log_rates = inputs
    length_here = log_rates.shape[-1]
    causal = jnp.arange(length_here)[:, None] >= jnp.arange(length_here)[None, :]
    running_totals = jnp.cumsum(log_rates, axis=-1)
    relative = running_totals[:, :, None] - running_totals[:, None, :]
    weight = jnp.where(causal[None], jnp.exp(jnp.where(causal[None], relative, 0.0)), 0.0)
    score_matrix = jnp.einsum('hqd,hkd->hqk', queries, key_matrix_rows, precision=exact_result) * weight
    carried_state = jnp.einsum('hqd,hdv->hqv', queries * jnp.exp(running_totals)[:, :, None], memory_state, precision=exact_result)
    output_rows = jnp.einsum('arf,afu->aru', score_matrix, value_matrix_rows, precision=exact_result) + carried_state
    decay_factors = jnp.exp(running_totals[:, -1:] - running_totals)
    memory_state = memory_state * jnp.exp(running_totals[:, -1])[:, None, None] + jnp.einsum('iwj,iwe->ije', key_matrix_rows * decay_factors[:, :, None], value_matrix_rows, precision=exact_result)
    return (memory_state, output_rows)

def reference(tokens, norm_gain, ret_query, ret_key, ret_value, att_query, att_key, att_value, log_decay, start_state, ret_gain, sink_logits, ret_out, att_out):

    def one_sequence(inputs):
        rows_in, decay_rows, initial = inputs
        as_float = rows_in.astype(jnp.float32)
        normed = (as_float * lax.rsqrt(lax.optimization_barrier(jnp.mean(as_float * as_float, axis=-1, keepdims=True)) + epsilon) * norm_gain).astype(jnp.bfloat16)

        def project(weights):
            return jnp.dot(normed, weights, preferred_element_type=jnp.float32).astype(jnp.bfloat16)
        ret_queries = project(ret_query)
        ret_keys = project(ret_key)
        ret_values = project(ret_value)
        att_queries = project(att_query)
        att_keys = project(att_key)
        att_values = project(att_value)
        positions = jnp.arange(SEQUENCE_LENGTH, dtype=jnp.int32)
        queries = rotate(ret_queries.astype(jnp.float32).reshape(SEQUENCE_LENGTH, RETENTION_HEADS, DK), positions)
        keys_rot = rotate(ret_keys.astype(jnp.float32).reshape(SEQUENCE_LENGTH, RETENTION_HEADS, DK), positions) * DK ** (-0.5)
        values_f = ret_values.astype(jnp.float32).reshape(SEQUENCE_LENGTH, RETENTION_HEADS, DV)
        count = SEQUENCE_LENGTH // BLOCK

        def blocked(array):
            return array.reshape(count, BLOCK, RETENTION_HEADS, array.shape[-1]).transpose(0, 2, 1, 3)
        log_rates = decay_rows.reshape(RETENTION_HEADS, count, BLOCK).transpose(1, 0, 2)
        _, pieces = lax.scan(block_step, initial, (blocked(queries), blocked(keys_rot), blocked(values_f), log_rates))
        retained = pieces.transpose(0, 2, 1, 3).reshape(SEQUENCE_LENGTH, RETENTION_HEADS, DV)
        centred = retained - lax.optimization_barrier(jnp.mean(retained, axis=-1, keepdims=True))
        variance = lax.optimization_barrier(jnp.mean(centred * centred, axis=-1, keepdims=True))
        ret_hidden = ((centred * lax.rsqrt(variance + epsilon)).reshape(SEQUENCE_LENGTH, RETENTION_HEADS * DV) * ret_gain).astype(jnp.bfloat16)
        windows = SEQUENCE_LENGTH // WINDOW
        groups = AQH // AKH
        grouped_q = att_queries.reshape(windows, WINDOW, AKH, groups, HD).astype(jnp.float32)

        def banded(array):
            blocks_now = array.reshape(windows, WINDOW, AKH, HD)
            earlier = jnp.concatenate([jnp.zeros((1, WINDOW, AKH, HD), array.dtype), blocks_now[:-1]], axis=0)
            return jnp.concatenate([earlier, blocks_now], axis=1).astype(jnp.float32)
        key_band = banded(att_keys)
        value_band = banded(att_values)
        score_matrix = jnp.einsum('nqhgd,nkhd->nhgqk', grouped_q, key_band) * HD ** (-0.5)
        query_index = WINDOW + jnp.arange(WINDOW)
        key_index = jnp.arange(2 * WINDOW)
        allowed = (key_index[None, :] <= query_index[:, None]) & (query_index[:, None] - key_index[None, :] < WINDOW)
        present = (jnp.arange(windows)[:, None] > 0) | (key_index >= WINDOW)[None, :]
        visible = (allowed[None] & present[:, None, :])[:, None, None]
        expo = jnp.exp(jnp.where(visible, score_matrix, -1e+30))
        summed = lax.optimization_barrier(jnp.sum(expo, axis=-1, keepdims=True)) + jnp.exp(sink_logits).reshape(1, AKH, groups, 1, 1)
        probs = (expo / summed).astype(jnp.bfloat16)
        att_hidden = jnp.einsum('nhgqk,nkhd->nqhgd', probs.astype(jnp.float32), value_band).astype(jnp.bfloat16).reshape(SEQUENCE_LENGTH, AQH * HD)
        ret_cols = RETENTION_HEADS * DV // N_TP
        att_cols = AQH * HD // N_TP
        mixed = jnp.zeros((SEQUENCE_LENGTH, D), jnp.float32)
        for group_index in range(N_TP):
            partial_value = jnp.dot(ret_hidden[:, group_index * ret_cols:(group_index + 1) * ret_cols], ret_out[group_index * ret_cols:(group_index + 1) * ret_cols], preferred_element_type=jnp.float32)
            partial_value = partial_value + jnp.dot(att_hidden[:, group_index * att_cols:(group_index + 1) * att_cols], att_out[group_index * att_cols:(group_index + 1) * att_cols], preferred_element_type=jnp.float32)
            rounded = lax.optimization_barrier(partial_value.astype(jnp.bfloat16))
            mixed = mixed + rounded.astype(jnp.float32)
        return mixed.astype(jnp.bfloat16)
    return lax.map(one_sequence, (tokens, log_decay, start_state))
```

```python
import jax
import jax.numpy as jnp
from jax import lax
from jax.sharding import PartitionSpec as P

DK = 256
DV = 256
HD = 64
WINDOW = 128

epsilon = 1e-06


def f32dot(a, b):
    return jnp.dot(a, b, preferred_element_type=jnp.float32)


def shift(array, distance, first=0):
    n = lax.axis_size("sp")
    if distance > 0:
        route = [(i, i + distance) for i in range(first, n - distance)]
    else:
        route = [(i, i + distance) for i in range(-distance, n - first)]
    return lax.ppermute(array, "sp", route)


def swap(array, mask, where=None):
    n, m = lax.axis_size("sp"), lax.axis_size("fs")
    chosen = range(n) if where is None else where
    route = [(i * m + f, i * m + (f ^ mask)) for i in chosen for f in range(m)]
    return lax.ppermute(array, ("sp", "fs"), route)


def core_swap(array):
    m = lax.axis_size("tp")
    return lax.ppermute(array, "tp", [(i, m - 1 - i) for i in range(m)])


def half_of(array, index, axis):
    size = array.shape[axis] // 2
    front = lax.slice_in_dim(array, 0, size, axis=axis)
    back = lax.slice_in_dim(array, size, 2 * size, axis=axis)
    return jnp.where(index == 0, front, back)


def shards(
    tokens,
    norm_gain,
    ret_query,
    ret_key,
    ret_value,
    att_query,
    att_key,
    att_value,
    log_decay,
    start_state,
    ret_gain,
    sink_logits,
    ret_out,
    att_out,
):
    n = lax.axis_size("sp")
    s, f, t = lax.axis_index("sp"), lax.axis_index("fs"), lax.axis_index("tp")
    a, b = f // 2, f % 2
    rows, feats = tokens.shape[1], tokens.shape[2]

    own_block = jnp.concatenate(
        [
            half_of(w, a, 1)
            for w in (ret_query, ret_key, ret_value, att_query, att_key, att_value)
        ],
        axis=1,
    )
    block_rows = own_block.shape[0]
    piece_rows = block_rows // 2
    mine = half_of(own_block, b, 0)

    own_tok = tokens[0]
    other_tok = swap(own_tok, 2)
    near = jnp.stack([own_tok, other_tok])
    far = jnp.stack([core_swap(own_tok), core_swap(other_tok)])
    near_f, far_f = near.astype(jnp.float32), far.astype(jnp.float32)
    mean = (
        jnp.sum(near_f * near_f, axis=-1, keepdims=True)
        + jnp.sum(far_f * far_f, axis=-1, keepdims=True)
    ) / (2 * feats)
    scale = lax.rsqrt(mean + epsilon)
    near_gain = half_of(norm_gain, t, 0)
    far_gain = half_of(norm_gain, 1 - t, 0)
    near_n = (near_f * scale * near_gain).astype(jnp.bfloat16).reshape(2 * rows, feats)
    far_n = (far_f * scale * far_gain).astype(jnp.bfloat16).reshape(2 * rows, feats)

    if piece_rows % 128 == 0:
        chunk_list = [
            lax.slice_in_dim(part, i * piece_rows, (i + 1) * piece_rows, axis=1)
            for part in (near_n, far_n)
            for i in range(n)
        ]
        chunks = jnp.stack(chunk_list)

        def features(block, half):
            return lax.dynamic_index_in_dim(
                chunks, (2 * block + half + n * t) % (2 * n), 0, keepdims=False
            )

        pieces = []
        up = down = mine
        for k in range(1, n):
            up, down = shift(up, 1, k - 1), shift(down, -1, k - 1)
            if 2 * k >= n:
                merged = jnp.where(s >= k, up, down)
                block = jnp.where(s >= k, s - k, s + k) % n
                valid = [i for i in range(n) if i >= k or i + k < n]
                pieces.append((block, merged, swap(merged, 1, valid)))
            else:
                pieces.append(((s - k) % n, up, swap(up, 1, range(k, n))))
                pieces.append(((s + k) % n, down, swap(down, 1, range(0, n - k))))
        total = f32dot(features(s, 0), own_block[:piece_rows]) + f32dot(
            features(s, 1), own_block[piece_rows:]
        )
        for block, here, there in pieces:
            total = total + f32dot(features(block, b), here)
            total = total + f32dot(features(block, 1 - b), there)
    else:
        here = lax.all_gather(mine, "sp", axis=0)
        there = swap(here, 1)
        whole = jnp.where(
            b == 0, jnp.stack([here, there], axis=1), jnp.stack([there, here], axis=1)
        ).reshape(2 * feats, own_block.shape[1])
        natural = jnp.where(
            t == 0,
            jnp.concatenate([near_n, far_n], axis=1),
            jnp.concatenate([far_n, near_n], axis=1),
        )
        total = f32dot(natural, whole)

    projected = total.astype(jnp.bfloat16).reshape(2, rows, own_block.shape[1])
    att_width = att_query.shape[1] // 2
    q_end, k_end, v_end = DK, 2 * DK, 2 * DK + DV
    rq, rk, rv = projected[..., :q_end], projected[..., q_end:k_end], projected[..., k_end:v_end]
    aq = projected[..., v_end : v_end + att_width]
    akv = projected[..., v_end + att_width :]

    positions = s * rows + jnp.arange(rows, dtype=jnp.int32)
    half_dim = DK // 2
    inverse = 1.0 / 10000.0 ** (jnp.arange(half_dim, dtype=jnp.float32) / half_dim)
    angles = positions.astype(jnp.float32)[:, None] * inverse[None, :]
    cosine, sine = jnp.cos(angles), jnp.sin(angles)

    def rotate(values):
        front = values[..., :half_dim].astype(jnp.float32)
        back = values[..., half_dim:].astype(jnp.float32)
        return jnp.concatenate(
            [front * cosine - back * sine, front * sine + back * cosine], axis=-1
        )

    rates = jnp.stack([half_of(log_decay[0], a, 0)[0], swap(half_of(log_decay[0], 1 - a, 0)[0], 2)])
    running = jnp.cumsum(rates, axis=-1)
    last = running[:, -1:]
    start_here = half_of(start_state[0], a, 0)[0].astype(jnp.bfloat16)
    start_there = swap(half_of(start_state[0], 1 - a, 0)[0].astype(jnp.bfloat16), 2, [0])
    start = jnp.stack([start_here, start_there]).astype(jnp.float32)

    keys = rotate(rk) * DK ** (-0.5)
    weighted_keys = (keys * jnp.exp(last - running)[:, :, None]).astype(jnp.bfloat16)
    local_state = jnp.einsum(
        "btd,btv->bdv", weighted_keys, rv, preferred_element_type=jnp.float32
    )
    incoming = jnp.where(s == 0, start, 0.0)
    local_state = local_state + jnp.exp(last)[:, :, None] * incoming
    covered = jnp.zeros_like(last)
    width = 0
    while width < n - 1:
        through = local_state if width == 0 else (
            local_state + jnp.exp(last)[:, :, None] * jnp.where(s == 0, 0.0, incoming)
        )
        arrived = shift(through.astype(jnp.bfloat16), width + 1).astype(jnp.float32)
        incoming = incoming + jnp.exp(covered)[:, :, None] * arrived
        if 2 * width + 1 < n - 1:
            covered = covered + shift(last + covered, width + 1)
        width = 2 * width + 1

    queries = rotate(rq)
    causal = jnp.arange(rows)[:, None] >= jnp.arange(rows)[None, :]
    relative = running[:, :, None] - running[:, None, :]
    decay = jnp.where(causal, jnp.exp(jnp.where(causal, relative, 0.0)), 0.0)
    scores = jnp.einsum(
        "bqd,bkd->bqk",
        queries.astype(jnp.bfloat16),
        keys.astype(jnp.bfloat16),
        preferred_element_type=jnp.float32,
    )
    inner = jnp.einsum(
        "bqk,bkv->bqv",
        (scores * decay).astype(jnp.bfloat16),
        rv,
        preferred_element_type=jnp.float32,
    )
    decayed_queries = (queries * jnp.exp(running)[:, :, None]).astype(jnp.bfloat16)

    edge = shift(akv[:, rows - WINDOW :], 1)
    extended = jnp.concatenate([edge, akv], axis=1)
    windows = rows // WINDOW
    band = jnp.stack(
        [extended[:, w * WINDOW : (w + 2) * WINDOW] for w in range(windows)], axis=1
    )
    key_band, value_band = band[..., :HD], band[..., HD:]
    groups = att_width // HD
    grouped = aq.reshape(2, windows, WINDOW, groups, HD)
    att_scores = jnp.einsum(
        "bwqgd,bwkd->bwgqk", grouped, key_band, preferred_element_type=jnp.float32
    ) * HD ** (-0.5)
    query_index = WINDOW + jnp.arange(WINDOW)
    key_index = jnp.arange(2 * WINDOW)
    allowed = (key_index[None, :] <= query_index[:, None]) & (
        query_index[:, None] - key_index[None, :] < WINDOW
    )
    key_place = s * rows - WINDOW + jnp.arange(windows)[:, None] * WINDOW + key_index[None, :]
    visible = (allowed[None] & (key_place >= 0)[:, None, :])[None, :, None]
    expo = jnp.exp(jnp.where(visible, att_scores, -1e30))
    sinks = jnp.exp(half_of(sink_logits, a, 0)).reshape(1, 1, groups, 1, 1)
    probs = (expo / (jnp.sum(expo, axis=-1, keepdims=True) + sinks)).astype(jnp.bfloat16)
    attended = jnp.einsum(
        "bwgqk,bwkd->bwqgd", probs, value_band, preferred_element_type=jnp.float32
    )
    att_hidden = attended.astype(jnp.bfloat16).reshape(2, rows, att_width)

    retained = inner + jnp.einsum(
        "bqd,bdv->bqv",
        decayed_queries,
        incoming.astype(jnp.bfloat16),
        preferred_element_type=jnp.float32,
    )
    centred = retained - jnp.mean(retained, axis=-1, keepdims=True)
    variance = jnp.mean(centred * centred, axis=-1, keepdims=True)
    gain = half_of(ret_gain, a, 0)
    ret_hidden = (centred * lax.rsqrt(variance + epsilon) * gain).astype(jnp.bfloat16)

    own_out = jnp.concatenate([ret_out, att_out], axis=0)
    side_out = swap(own_out, 1)
    over_out = swap(own_out, 2)
    cross_out = swap(side_out, 2)
    hidden = jnp.concatenate([ret_hidden, att_hidden], axis=-1)
    theirs = swap(hidden[1], 2)
    ours = hidden[0]
    ordered = jnp.where(
        a == 0,
        jnp.concatenate([ours[:, :DV], theirs[:, :DV], ours[:, DV:], theirs[:, DV:]], axis=1),
        jnp.concatenate([theirs[:, :DV], ours[:, :DV], theirs[:, DV:], ours[:, DV:]], axis=1),
    )
    own_p, side_p, over_p, cross_p = (
        f32dot(ordered, w).astype(jnp.bfloat16) for w in (own_out, side_out, over_out, cross_out)
    )

    def in_order(first, second):
        return jnp.where(
            b == 0,
            jnp.concatenate([first, second], axis=1),
            jnp.concatenate([second, first], axis=1),
        )

    half_a, half_other = in_order(own_p, side_p), in_order(over_p, cross_p)
    kept = jnp.where(a == t, half_a, half_other)
    given = jnp.where(a == t, half_other, half_a)
    mixed = kept.astype(jnp.float32) + core_swap(given).astype(jnp.float32)
    return mixed.astype(jnp.bfloat16)[None]


def solution(mesh):
    placed = (
        P("fs", "sp", "tp"),
        P(),
        P("sp", "tp"),
        P("sp", "tp"),
        P("sp", "tp"),
        P("sp", "tp"),
        P("sp", "tp"),
        P("sp", "tp"),
        P("fs", "tp", "sp"),
        P("fs", "tp", None, None),
        P("tp"),
        P("tp"),
        P("tp", "fs"),
        P("tp", "fs"),
    )
    return jax.shard_map(
        shards, mesh=mesh, in_specs=placed, out_specs=P("fs", "sp", "tp"), check_vma=False
    )
```
